32 devices in a mesh: sp: 8 (over z, x), dp: 4 (over y, core).
Axes of the slice: x: 2, y: 2, z: 4, core: 2. Of those that a mesh axis runs over, the one named last changes fastest.
Arguments:
- queries: bfloat16 [4, 1024, 2048], P('dp', 'sp'), may hold values from -12 to 12
- key_rows: bfloat16 [4, 1024, 2048], P('dp', 'sp'), may hold values from -12 to 12
- value_rows: bfloat16 [4, 1024, 2048], P('dp', 'sp'), may hold values from -6 to 6
- lambdas: float32 [16], P('sp'), may hold values from 0.3 to 0.8
- head_gain: float32 [128], replicated, may hold values from 0.1 to 1.9
- out_weight: bfloat16 [2048, 2048], replicated, may hold values from -0.125 to 0.125
- residual: bfloat16 [4, 1024, 2048], P('dp', 'sp'), may hold values from -6 to 6
- mixer_gain: float32 [2048], replicated, may hold values from 0.1 to 1.9
- channel_gain: float32 [2048], replicated, may hold values from 0.1 to 1.9
- expert_gain: float32 [2048], replicated, may hold values from 0.1 to 1.9
- routes: int32 [4, 1024, 2], P('dp', 'sp'), may hold values from 0 to 7, all different within a row; in each aligned block of 128 rows (0 to 127, 128 to 255, ..., all dimensions but the last counted through in order) at most 48 rows name the same one
- route_logits: float32 [4, 1024, 2], P('dp', 'sp'), may hold values from -5 to 5
- gate_weight: bfloat16 [8, 2048, 4096], P('sp', None, 'dp'), may hold values from -0.125 to 0.125
- up_weight: bfloat16 [8, 2048, 4096], P('sp', None, 'dp'), may hold values from -0.125 to 0.125
- down_weight: bfloat16 [8, 4096, 2048], P('sp', 'dp'), may hold values from -0.09375 to 0.09375
Outputs:
- updated: bfloat16 [4, 1024, 2048], P('dp', 'sp')
The draws below stay inside these ranges and needn't reach their ends.
Inputs may be any that keep to these rules, and one draw needn't show every extreme that they name: `routes`: among the rows of one device no expert is named by more than 48 rows; in some of these blocks one expert is named by exactly 48.
All inputs are finite; a program needn't handle non-finite values.
Results may differ from the reference program's by a relative error of at most 0.014.
Values may be sent and summed in bfloat16 or wider, within the bound.
No kernel may reach another device: no remote copies, remote signals or barrier semaphores. Data moves between devices by JAX's collectives and lax.ppermute only.
A program may use at most 128 MiB of HBM per device.

```python
import math
import jax
import jax.numpy as jnp
import numpy as np
from jax import lax

D = 2048
HEADS = 16
HD = 64
FF = 4096
TOP = 2
TOK_DEV = 128
LEN = 1024
SEQS = 4
EXPERTS = 8
CAP = 48
N_SP = 8
N_DP = 4


def draw_queries(key, part):
    base = jnp.clip(1.32 * jax.random.normal(jax.random.fold_in(key, 1), (SEQS, LEN, HEADS * 2 * HD), jnp.float32), -12.0, 12.0)
    return base.astype(jnp.bfloat16)


def draw_key_rows(key, part):
    base = jnp.clip(1.32 * jax.random.normal(jax.random.fold_in(key, 2), (SEQS, LEN, HEADS * 2 * HD), jnp.float32), -12.0, 12.0)
    return base.astype(jnp.bfloat16)


def block_scale(stream_key, shape, cuts, low, top_value):
    factor_of, own = 1.0, jax.random.fold_in(stream_key, 6)
    for position, parts in cuts:
        steps = jnp.exp(jax.random.uniform(jax.random.fold_in(own, position), (parts,), jnp.float32, low / len(cuts), top_value / len(cuts)))
        factor_of = factor_of * jnp.repeat(steps, shape[position] // parts).reshape([-1 if axis == position else 1 for axis in range(len(shape))])
    return factor_of


def routed_block(rng, own, number, rows, count, top, most, skew):
    ranking = jax.random.permutation(rng, count)
    heavy_load, usual = load_shares(count, rows * top, most, skew, True), load_shares(count, rows * top, most, skew, False)
    places = jnp.arange(count)

    def named(sizes, turn):
        used = int((sizes > 0).sum())
        fixed = max(1, used // 4)
        passed = fixed + (places - fixed + turn * (used - fixed)) % max(1, count - fixed)
        return jnp.zeros((count,), jnp.int32).at[ranking[jnp.where(places < fixed, places, passed)]].set(jnp.asarray(sizes, jnp.int32))

    sizes = jnp.where(number % 4 == 0, named(heavy_load, number // 4), named(usual, number - number // 4 - 1))
    mixed = jax.random.permutation(jax.random.fold_in(own, 3), count)
    giver, receiver = mixed[0:count // 2 * 2:2], mixed[1:count // 2 * 2:2]
    slack = jnp.minimum(sizes[giver] - 1, most - sizes[receiver]) // 2
    slack = jnp.where((giver == ranking[0]) | (receiver == ranking[0]) | (sizes[receiver] == 0), 0, jnp.maximum(slack, 0))
    passed = jax.random.randint(jax.random.fold_in(own, 4), (count // 2,), 0, 1 << 20) % (slack + 1)
    sizes = sizes.at[giver].add(-passed).at[receiver].add(passed)
    labels = jnp.searchsorted(jnp.cumsum(sizes), jnp.arange(rows * top), side="right").astype(jnp.int32)
    table = labels.reshape(top, rows).T
    table = table[jax.random.permutation(jax.random.fold_in(own, 1), rows)]
    turn = jax.random.randint(jax.random.fold_in(own, 2), (rows, 1), 0, top)
    return jnp.take_along_axis(table, (jnp.arange(top)[None, :] + turn) % top, axis=1)


def load_shares(number_of, total, most, lean, full):
    loads = [(1 << 20) // math.isqrt(grade ** lean) + 1 for grade in range(1, number_of + 1)]
    largest = most if full else min(most, max(-(-total // number_of), total * loads[0] // sum(loads)))
    least = 1 if total - largest >= number_of - 1 else 0
    holding, rest = [largest] + [least] * (number_of - 1), total - largest - least * (number_of - 1)
    while rest > 0:
        free = [i for i in range(1, number_of) if holding[i] < largest] or [i for i in range(1, number_of) if holding[i] < most]
        mass, left = sum([loads[i] for i in free]), rest
        for i in free:
            more = min(most - holding[i], max(1, left * loads[i] // mass), rest)
            holding[i] = holding[i] + more
            rest = rest - more
    return np.array(holding)


def scatter_about(key, shape, deviation, reach, pieces=(), kind=jnp.bfloat16):
    values = deviation * jax.random.normal(key, shape, jnp.float32)
    if pieces:
        values = values * block_scale(key, shape, pieces, -0.22, 0.18)
    return jnp.clip(values, -reach, reach).astype(kind)


def setup_inputs(seed: int = 0) -> dict:
    seeds = jax.random.split(jax.random.key(seed), 16)
    queries = draw_queries(jax.random.fold_in(seeds[15], 71), 0)
    key_rows = draw_key_rows(jax.random.fold_in(seeds[15], 71), 0)
    value_rows = scatter_about(seeds[2], (SEQS, LEN, HEADS * 2 * HD), 1.0, 6.0, ((0, 4), (1, 8)))
    lambdas = jnp.clip(0.3 + 0.5 * jax.random.uniform(seeds[3], (HEADS,), jnp.float32) ** block_scale(seeds[3], (HEADS,), ((0, 8),), -0.2, 0.2), 0.3, 0.8)
    head_gain = jnp.clip(1.0 + 0.18 * jax.random.normal(seeds[4], (2 * HD,), jnp.float32), 0.1, 1.9)
    out_weight = scatter_about(seeds[5], (HEADS * 2 * HD, D), (HEADS * 2 * HD) ** -0.5, 0.125)
    residual = scatter_about(seeds[6], (SEQS, LEN, D), 1.0, 6.0, ((0, 4), (1, 8)))
    mixer_gain = jnp.clip(1.0 + 0.18 * jax.random.normal(seeds[7], (D,), jnp.float32), 0.1, 1.9)
    channel_gain = jnp.clip(1.0 + 0.18 * jax.random.normal(seeds[8], (D,), jnp.float32), 0.1, 1.9)
    expert_gain = jnp.clip(1.0 + 0.18 * jax.random.normal(seeds[9], (D,), jnp.float32), 0.1, 1.9)
    routes_keys = jax.random.split(jax.random.fold_in(seeds[10], 1), SEQS * LEN // TOK_DEV)
    routes_turns = jax.random.permutation(jax.random.fold_in(seeds[10], 3), SEQS * LEN // TOK_DEV)
    routes = jax.vmap(lambda own, number: routed_block(jax.random.fold_in(seeds[10], 2), own, number, TOK_DEV, EXPERTS, TOP, CAP, 2))(routes_keys, routes_turns).reshape((SEQS, LEN, TOP))
    route_logits = scatter_about(seeds[11], (SEQS, LEN, TOP), 1.0, 5.0, ((0, 4), (1, 8)), jnp.float32)
    gate_weight = scatter_about(seeds[12], (EXPERTS, D, FF), D ** -0.5, 0.125, ((0, 8), (2, 4)))
    up_weight = scatter_about(seeds[13], (EXPERTS, D, FF), D ** -0.5, 0.125, ((0, 8), (2, 4)))
    down_weight = scatter_about(seeds[14], (EXPERTS, FF, D), FF ** -0.5, 0.09375, ((0, 8), (1, 4)))
    return {"queries": queries, "key_rows": key_rows, "value_rows": value_rows, "lambdas": lambdas, "head_gain": head_gain, "out_weight": out_weight, "residual": residual, "mixer_gain": mixer_gain, "channel_gain": channel_gain, "expert_gain": expert_gain, "routes": routes, "route_logits": route_logits, "gate_weight": gate_weight, "up_weight": up_weight, "down_weight": down_weight}


def rotate(field):
    dim_full = field.shape[-1]
    dim_half = dim_full // 2
    inverse = 1.0 / 10000.0 ** (jnp.arange(0, dim_full, 2, dtype=jnp.float32) / dim_full)
    angles = jnp.arange(field.shape[-4], dtype=jnp.float32)[:, None] * inverse[None, :]
    cosine = jnp.cos(angles)[:, None, None, :]
    sine_table = jnp.sin(angles)[:, None, None, :]
    floats = field.astype(jnp.float32)
    front_part = floats[..., :dim_half]
    second = floats[..., dim_half:]
    turned = jnp.concatenate([front_part * cosine - second * sine_table, second * cosine + front_part * sine_table], axis=-1)
    return turned.astype(jnp.bfloat16)

def rms_scale(values, epsilon):
    return values * lax.rsqrt(lax.optimization_barrier(jnp.mean(values * values, axis=-1, keepdims=True)) + epsilon)

def reference(queries, key_rows, value_rows, lambdas, head_gain, out_weight, residual, mixer_gain, channel_gain, expert_gain, routes, route_logits, gate_weight, up_weight, down_weight):
    seq_count = queries.shape[0]
    length = queries.shape[1]
    query_rot = rotate(queries.reshape(seq_count, length, HEADS, 2, HD))
    keys_rot = rotate(key_rows.reshape(seq_count, length, HEADS, 2, HD))
    query_items = query_rot.transpose(0, 2, 1, 3, 4).reshape(seq_count * HEADS, length, 2, HD)
    key_items = keys_rot.transpose(0, 2, 1, 3, 4).reshape(seq_count * HEADS, length, 2, HD)
    value_items = value_rows.reshape(seq_count, length, HEADS, 2 * HD).transpose(0, 2, 1, 3).reshape(seq_count * HEADS, length, 2 * HD)
    lambda_items = jnp.tile(lambdas, seq_count)

    def one_head(item):
        query_one, key_one, value_one, lambda_one = item
        scores = jnp.einsum('qcd,kcd->cqk', query_one.astype(jnp.float32), key_one.astype(jnp.float32)) * HD ** (-0.5)
        probs = jax.nn.softmax(scores, axis=-1)
        mixing = (probs[0] - lambda_one * probs[1]).astype(jnp.bfloat16)
        head_mix = jnp.dot(mixing, value_one, preferred_element_type=jnp.float32)
        return (rms_scale(head_mix, 1e-05) * head_gain).astype(jnp.bfloat16)
    heads_out = lax.map(one_head, (query_items, key_items, value_items, lambda_items))
    attended = heads_out.reshape(seq_count, HEADS, length, 2 * HD).transpose(0, 2, 1, 3).reshape(seq_count * length, HEADS * 2 * HD)
    projected = jnp.dot(attended, out_weight, preferred_element_type=jnp.float32)
    stream = (residual.reshape(seq_count * length, D).astype(jnp.float32) + rms_scale(projected, 1e-06) * mixer_gain).astype(jnp.bfloat16)
    normed = (rms_scale(stream.astype(jnp.float32), 1e-06) * channel_gain).astype(jnp.bfloat16)
    choice_ids = routes.reshape(-1).astype(jnp.int32)
    token_of = jnp.arange(choice_ids.shape[0], dtype=jnp.int32) // TOP
    shares = jax.nn.softmax(route_logits.reshape(-1, TOP), axis=-1).reshape(-1)
    limit = N_SP * N_DP * CAP
    block_units = FF // N_DP

    def per_expert(total, expert):
        others = (choice_ids != expert).astype(jnp.int32)
        order = jnp.argsort(others, stable=True)[:limit].astype(jnp.int32)
        count = jnp.sum(1 - others)
        valid = (jnp.arange(limit, dtype=jnp.int32) < count).astype(jnp.float32)
        tok_index = token_of[order]
        rows = normed[tok_index]
        gate_act = jnp.dot(rows, gate_weight[expert], preferred_element_type=jnp.float32)
        up_act = jnp.dot(rows, up_weight[expert], preferred_element_type=jnp.float32)
        hidden = (jax.nn.silu(gate_act) * up_act).astype(jnp.bfloat16)
        expert_sum = jnp.zeros((limit, D), jnp.float32)
        for block in range(N_DP):
            part = jnp.dot(hidden[:, block * block_units:(block + 1) * block_units], down_weight[expert, block * block_units:(block + 1) * block_units], preferred_element_type=jnp.float32)
            expert_sum = expert_sum + lax.optimization_barrier(part.astype(jnp.bfloat16)).astype(jnp.float32)
        expert_out = expert_sum.astype(jnp.bfloat16).astype(jnp.float32)
        weighted = expert_out * (shares[order] * valid)[:, None]
        return (total.at[tok_index].add(weighted), None)
    combined, _ = lax.scan(per_expert, jnp.zeros((seq_count * length, D), jnp.float32), jnp.arange(EXPERTS, dtype=jnp.int32))
    updated = stream.astype(jnp.float32) + rms_scale(combined, 1e-06) * expert_gain
    return updated.astype(jnp.bfloat16).reshape(seq_count, length, D)
```

```python
import functools
import math

import jax
import jax.numpy as jnp
from jax import lax
from jax.experimental import pallas as pl
from jax.experimental.pallas import tpu as pltpu
from jax.sharding import PartitionSpec as P


F32 = jnp.float32
BF16 = jnp.bfloat16


def params(**kwargs):
    return pltpu.CompilerParams(vmem_limit_bytes=56 * 1024 * 1024, **kwargs)


def layout_kernel(cos_ref, sin_ref, q_ref, k_ref, v_ref, *out_refs, scale):
    heads = len(out_refs)
    width = cos_ref.shape[1]
    groups = q_ref.shape[1] // (heads * width)
    quarter = width // 4
    cosine = cos_ref[...]
    signed_sine = sin_ref[...]
    lane = lax.broadcasted_iota(jnp.int32, cosine.shape, 1)
    front = (lane % (width // 2)) < quarter

    def turn(x, factor):
        x = x.astype(F32)
        partner = jnp.where(front, pltpu.roll(x, width - quarter, 1), pltpu.roll(x, quarter, 1))
        return (x * cosine + partner * signed_sine).astype(BF16) * factor

    for g in range(groups):
        for j in range(heads):
            at = pl.ds((g * heads + j) * width, width)
            out_refs[j][g, :, 0:width] = turn(q_ref[:, at], jnp.asarray(scale, BF16))
            out_refs[j][g, :, width : 2 * width] = turn(k_ref[:, at], jnp.asarray(1.0, BF16))
            out_refs[j][g, :, 2 * width : 3 * width] = v_ref[:, at]


def attention_kernel(lam_ref, gain_ref, q_ref, k_ref, v_ref, o_ref, *, head):
    width = q_ref.shape[1]
    rows = q_ref.shape[0]
    q = q_ref[...]
    lane = lax.broadcasted_iota(jnp.int32, q.shape, 1)
    zero = jnp.zeros_like(q)
    both = jnp.concatenate(
        [jnp.where(lane < width // 2, q, zero), jnp.where(lane < width // 2, zero, q)], axis=0
    )
    scores = lax.dot_general(
        both, k_ref[...], (((1,), (1,)), ((), ())), preferred_element_type=F32
    )
    top = jnp.max(scores, axis=1, keepdims=True)
    weights = jnp.exp(scores - top).astype(BF16)
    values = v_ref[...]
    extended = jnp.concatenate([values, jnp.ones_like(values)], axis=1)
    mixed = jnp.dot(weights, extended, preferred_element_type=F32)
    ratio = mixed[:, :width] / mixed[:, width:]
    out = ratio[:rows] - lam_ref[head] * ratio[rows:]
    norm = lax.rsqrt(jnp.mean(out * out, axis=1, keepdims=True) + 1e-05)
    o_ref[...] = (out * norm * gain_ref[...]).astype(BF16)


def rms(x, epsilon):
    return x * lax.rsqrt(jnp.mean(x * x, axis=1, keepdims=True) + epsilon)


def project_kernel(*refs, heads, chunks, experts):
    head_refs = refs[:heads]
    w_ref, res_ref, mg_ref, cg_ref, routes_ref, stream_ref = refs[heads : heads + 6]
    out_refs = refs[heads + 6 : heads + 6 + chunks]
    acc_ref = refs[-1]
    step = pl.program_id(0)
    width = head_refs[0].shape[2]
    per_step = w_ref.shape[0] // (heads * width)
    lhs = jnp.concatenate(
        [head_refs[j][step * per_step + g] for g in range(per_step) for j in range(heads)], axis=1
    )
    update = jnp.dot(lhs, w_ref[...], preferred_element_type=F32)

    @pl.when(step == 0)
    def _():
        acc_ref[...] = update

    @pl.when(step != 0)
    def _():
        acc_ref[...] += update

    @pl.when(step == pl.num_programs(0) - 1)
    def _():
        stream = (res_ref[...].astype(F32) + rms(acc_ref[...], 1e-06) * mg_ref[...]).astype(BF16)
        stream_ref[...] = stream
        normed = (rms(stream.astype(F32), 1e-06) * cg_ref[...]).astype(BF16)
        tokens = stream.shape[0]
        expert_id = lax.broadcasted_iota(jnp.int32, (experts, tokens), 0)
        named = expert_id == routes_ref[0:1, :]
        for j in range(1, routes_ref.shape[0]):
            named = named | (expert_id == routes_ref[j : j + 1, :])
        before = lax.broadcasted_iota(jnp.int32, (tokens, tokens), 0) < lax.broadcasted_iota(
            jnp.int32, (tokens, tokens), 1
        )
        rank = jnp.dot(
            named.astype(F32).astype(BF16),
            before.astype(F32).astype(BF16),
            preferred_element_type=F32,
        )
        rank = jnp.where(named, rank, -1.0)
        slots = out_refs[0].shape[0] // experts
        for c in range(chunks):
            slot = (
                lax.broadcasted_iota(jnp.int32, (slots, tokens), 0).astype(F32) + float(c * slots)
            )
            select = jnp.concatenate(
                [(slot == rank[e : e + 1, :]).astype(F32) for e in range(experts)], axis=0
            ).astype(BF16)
            out_refs[c][...] = jnp.dot(select, normed, preferred_element_type=F32).astype(BF16)


def expert_kernel(*refs, pieces):
    x_refs = refs[:pieces]
    g_ref, u_ref, d_ref, mine_ref, theirs_ref, rows_ref, acc_ref = refs[pieces:]
    step = pl.program_id(0)
    size = x_refs[0].shape[0]

    @pl.when(step == 0)
    def _():
        for i in range(pieces):
            rows_ref[i * size : (i + 1) * size, :] = x_refs[i][...]

    rows = rows_ref[...]
    gate = jnp.dot(rows, g_ref[0], preferred_element_type=F32)
    up = jnp.dot(rows, u_ref[0], preferred_element_type=F32)
    hidden = (gate / (1.0 + jnp.exp(-gate)) * up).astype(BF16)
    update = jnp.dot(hidden, d_ref[0], preferred_element_type=F32)

    @pl.when(step == 0)
    def _():
        acc_ref[...] = update

    @pl.when(step != 0)
    def _():
        acc_ref[...] += update

    @pl.when(step == pl.num_programs(0) - 1)
    def _():
        half = pieces // 2
        for i in range(half):
            mine_ref[i] = acc_ref[i * size : (i + 1) * size, :].astype(BF16)
            theirs_ref[i] = acc_ref[(half + i) * size : (half + i + 1) * size, :].astype(BF16)


def combine_kernel(*refs, chunks, experts):
    back_refs = refs[:chunks]
    stream_ref, routes_ref, logits_ref, gain_ref, out_ref = refs[chunks:]
    tokens = stream_ref.shape[0]
    top = routes_ref.shape[1]
    slots = back_refs[0].shape[0] // experts
    expert_id = lax.broadcasted_iota(jnp.int32, (tokens, experts), 1)
    hits = [expert_id == routes_ref[:, j : j + 1] for j in range(top)]
    named = functools.reduce(jnp.logical_or, hits)
    after = lax.broadcasted_iota(jnp.int32, (tokens, tokens), 1) < lax.broadcasted_iota(
        jnp.int32, (tokens, tokens), 0
    )
    rank = jnp.dot(
        after.astype(F32).astype(BF16), named.astype(F32).astype(BF16), preferred_element_type=F32
    )
    logits = logits_ref[...]
    powers = jnp.exp(logits - jnp.max(logits, axis=1, keepdims=True))
    shares = powers / jnp.sum(powers, axis=1, keepdims=True)
    combined = None
    for j in range(top):
        slot = jnp.sum(jnp.where(hits[j], rank, 0.0), axis=1, keepdims=True).astype(jnp.int32)
        place = routes_ref[:, j : j + 1] * (slots * chunks) + slot
        picked = None
        for c in range(chunks):
            column = lax.broadcasted_iota(jnp.int32, (tokens, experts * slots), 1)
            home = (column // slots) * (slots * chunks) + column % slots + c * slots
            select = (home == place).astype(F32).astype(BF16)
            got = jnp.dot(select, back_refs[c][...], preferred_element_type=F32)
            picked = got if picked is None else picked + got
        picked = picked * shares[:, j : j + 1]
        combined = picked if combined is None else combined + picked
    out_ref[...] = (stream_ref[...].astype(F32) + rms(combined, 1e-06) * gain_ref[...]).astype(BF16)


def local(
    queries,
    key_rows,
    value_rows,
    lambdas,
    head_gain,
    out_weight,
    residual,
    mixer_gain,
    channel_gain,
    expert_gain,
    routes,
    route_logits,
    gate_weight,
    up_weight,
    down_weight,
):
    sp_count = lax.axis_size("sp")
    dp_count = lax.axis_size("dp")
    heads = lambdas.shape[0]
    width = head_gain.shape[0]
    head_dim = width // 2
    tokens, model_dim = residual.shape[1:]
    all_width = queries.shape[2]
    length = tokens * sp_count
    scale = head_dim**-0.5

    lane = jnp.arange(width)
    inverse = 1.0 / 10000.0 ** (
        (2 * (lane % (head_dim // 2))).astype(F32) / head_dim
    )
    position = lax.axis_index("sp") * tokens + jnp.arange(tokens)
    angles = position.astype(F32)[:, None] * inverse[None, :]
    cosine = jnp.cos(angles)
    signed_sine = jnp.where((lane % head_dim < head_dim // 2)[None, :], -1.0, 1.0) * jnp.sin(angles)

    lay_steps = 4
    lay_groups = sp_count // lay_steps
    columns = pl.BlockSpec((None, tokens, all_width // lay_steps), lambda i: (0, 0, i))
    table = pl.BlockSpec((tokens, width), lambda i: (0, 0))
    outgoing = pl.pallas_call(
        functools.partial(layout_kernel, scale=scale),
        grid=(lay_steps,),
        in_specs=[table, table, columns, columns, columns],
        out_specs=[
            pl.BlockSpec((lay_groups, tokens, 3 * width), lambda i: (i, 0, 0))
            for _ in range(heads)
        ],
        out_shape=[
            jax.ShapeDtypeStruct((sp_count, tokens, 3 * width), BF16) for _ in range(heads)
        ],
        compiler_params=params(),
        name="lay",
    )(cosine, signed_sine, queries, key_rows, value_rows)

    gain_row = head_gain.reshape(1, width)
    block = math.gcd(length, 256)
    token_heads = []
    for j in range(heads):
        arrived = lax.all_to_all(outgoing[j], "sp", split_axis=0, concat_axis=0, tiled=True)
        arrived = arrived.reshape(length, 3 * width)
        head_out = pl.pallas_call(
            functools.partial(attention_kernel, head=j),
            grid=(length // block,),
            in_specs=[
                pl.BlockSpec(memory_space=pltpu.SMEM),
                pl.BlockSpec((1, width), lambda i: (0, 0)),
                pl.BlockSpec((block, width), lambda i: (i, 0)),
                pl.BlockSpec((length, width), lambda i: (0, 1)),
                pl.BlockSpec((length, width), lambda i: (0, 2)),
            ],
            out_specs=pl.BlockSpec((block, width), lambda i: (i, 0)),
            out_shape=jax.ShapeDtypeStruct((length, width), BF16),
            compiler_params=params(),
            cost_estimate=pl.CostEstimate(
                flops=8 * length * length * width,
                bytes_accessed=8 * length * width,
                transcendentals=2 * length * length,
            ),
            name=f"attend{j}",
        )(lambdas, gain_row, arrived, arrived, arrived)
        token_heads.append(
            lax.all_to_all(
                head_out.reshape(sp_count, tokens, width),
                "sp",
                split_axis=0,
                concat_axis=0,
                tiled=True,
            )
        )

    experts = sp_count * gate_weight.shape[0]
    capacity = max(2, 3 * tokens // experts)
    slots = next((n for n in (16, 8) if capacity % n == 0), capacity)
    chunks = capacity // slots
    size = experts * slots
    top = routes.shape[2]
    steps = 4
    k_rows = all_width // steps
    row_spec = pl.BlockSpec((1, model_dim), lambda i: (0, 0))
    full = pl.BlockSpec((tokens, model_dim), lambda i: (0, 0))
    results = pl.pallas_call(
        functools.partial(project_kernel, heads=heads, chunks=chunks, experts=experts),
        grid=(steps,),
        in_specs=[pl.BlockSpec((sp_count, tokens, width), lambda i: (0, 0, 0))] * heads
        + [
            pl.BlockSpec((k_rows, model_dim), lambda i: (i, 0)),
            full,
            row_spec,
            row_spec,
            pl.BlockSpec((top, tokens), lambda i: (0, 0)),
        ],
        out_specs=[full] + [pl.BlockSpec((size, model_dim), lambda i: (0, 0))] * chunks,
        out_shape=[jax.ShapeDtypeStruct((tokens, model_dim), BF16)]
        + [jax.ShapeDtypeStruct((size, model_dim), BF16)] * chunks,
        scratch_shapes=[pltpu.VMEM((tokens, model_dim), F32)],
        compiler_params=params(),
        cost_estimate=pl.CostEstimate(
            flops=2 * tokens * all_width * model_dim,
            bytes_accessed=2 * all_width * model_dim,
            transcendentals=0,
        ),
        name="project",
    )(
        *token_heads,
        out_weight,
        residual.reshape(tokens, model_dim),
        mixer_gain.reshape(1, model_dim),
        channel_gain.reshape(1, model_dim),
        routes.reshape(tokens, top).T,
    )
    stream, sent = results[0], results[1:]

    rows_y = dp_count // 2
    core_swap = [(i, i ^ 1) for i in range(dp_count)]

    def shift(k):
        return [(i, ((i // 2 + k) % rows_y) * 2 + i % 2) for i in range(dp_count)]

    pieces = 2 * rows_y
    hidden = gate_weight.shape[2]
    f_steps = 4
    f_block = hidden // f_steps

    def dispatch(rows):
        return lax.all_to_all(
            rows.reshape(sp_count, slots, model_dim), "sp", split_axis=0, concat_axis=0, tiled=True
        ).reshape(size, model_dim)

    def spread(rows):
        here = [rows] + [lax.ppermute(rows, "dp", shift(k)) for k in range(1, rows_y)]
        return here + [lax.ppermute(r, "dp", core_swap) for r in here]

    def expert(rows):
        return pl.pallas_call(
            functools.partial(expert_kernel, pieces=pieces),
            grid=(f_steps,),
            in_specs=[pl.BlockSpec((size, model_dim), lambda i: (0, 0))] * pieces
            + [
                pl.BlockSpec((1, model_dim, f_block), lambda i: (0, 0, i)),
                pl.BlockSpec((1, model_dim, f_block), lambda i: (0, 0, i)),
                pl.BlockSpec((1, f_block, model_dim), lambda i: (0, i, 0)),
            ],
            out_specs=[pl.BlockSpec((rows_y, size, model_dim), lambda i: (0, 0, 0))] * 2,
            out_shape=[jax.ShapeDtypeStruct((rows_y, size, model_dim), BF16)] * 2,
            scratch_shapes=[
                pltpu.VMEM((pieces * size, model_dim), BF16),
                pltpu.VMEM((pieces * size, model_dim), F32),
            ],
            compiler_params=params(),
            cost_estimate=pl.CostEstimate(
                flops=6 * pieces * size * model_dim * hidden,
                bytes_accessed=6 * model_dim * hidden,
                transcendentals=pieces * size * hidden,
            ),
            name="expert",
        )(*rows, gate_weight, up_weight, down_weight)

    def gather_sums(mine, theirs):
        other = lax.ppermute(theirs, "dp", core_swap)
        pair = mine.astype(F32) + other.astype(F32)
        total = pair[0]
        for k in range(1, rows_y):
            total = total + lax.ppermute(pair[k].astype(BF16), "dp", shift(rows_y - k)).astype(F32)
        total = total.astype(BF16)
        return lax.all_to_all(
            total.reshape(sp_count, slots, model_dim), "sp", split_axis=0, concat_axis=0, tiled=True
        ).reshape(size, model_dim)

    dispatched = [dispatch(r) for r in sent]
    spreads = [spread(r) for r in dispatched]
    parts = [expert(r) for r in spreads]
    returned = [gather_sums(*p) for p in parts]

    updated = pl.pallas_call(
        functools.partial(combine_kernel, chunks=chunks, experts=experts),
        out_shape=jax.ShapeDtypeStruct((tokens, model_dim), BF16),
        compiler_params=params(),
        name="combine",
    )(
        *returned,
        stream,
        routes.reshape(tokens, top),
        route_logits.reshape(tokens, top),
        expert_gain.reshape(1, model_dim),
    )
    return updated.reshape(1, tokens, model_dim)


def solution(mesh):
    placed = (
        P("dp", "sp", None),
        P("dp", "sp", None),
        P("dp", "sp", None),
        P("sp"),
        P(),
        P(),
        P("dp", "sp", None),
        P(),
        P(),
        P(),
        P("dp", "sp", None),
        P("dp", "sp", None),
        P("sp", None, "dp"),
        P("sp", None, "dp"),
        P("sp", "dp", None),
    )
    return jax.shard_map(
        local, mesh=mesh, in_specs=placed, out_specs=P("dp", "sp", None), check_vma=False
    )
```

```python
import functools
import math

import jax
import jax.numpy as jnp
from jax import lax
from jax.experimental import pallas as pl
from jax.experimental.pallas import tpu as pltpu
from jax.sharding import PartitionSpec as P


F32 = jnp.float32
BF16 = jnp.bfloat16


def params(megabytes=24, **kwargs):
    return pltpu.CompilerParams(vmem_limit_bytes=megabytes * 1024 * 1024, **kwargs)


def on_chip(x):
    return pltpu.with_memory_space_constraint(x, pltpu.VMEM)


def layout_kernel(cos_ref, sin_ref, q_ref, k_ref, v_ref, *out_refs, scale):
    heads = len(out_refs)
    width = cos_ref.shape[1]
    groups = q_ref.shape[1] // (heads * width)
    quarter = width // 4
    cosine = cos_ref[...]
    signed_sine = sin_ref[...]
    lane = lax.broadcasted_iota(jnp.int32, cosine.shape, 1)
    front = (lane % (width // 2)) < quarter

    def turn(x, factor):
        x = x.astype(F32)
        partner = jnp.where(front, pltpu.roll(x, width - quarter, 1), pltpu.roll(x, quarter, 1))
        return (x * cosine + partner * signed_sine).astype(BF16) * factor

    for g in range(groups):
        for j in range(heads):
            at = pl.ds((g * heads + j) * width, width)
            out_refs[j][g, :, 0:width] = turn(q_ref[:, at], jnp.asarray(scale, BF16))
            out_refs[j][g, :, width : 2 * width] = turn(k_ref[:, at], jnp.asarray(1.0, BF16))
            out_refs[j][g, :, 2 * width : 3 * width] = v_ref[:, at]


def attention_kernel(lam_ref, gain_ref, q_ref, k_ref, v_ref, o_ref, *, head):
    width = q_ref.shape[1]
    rows = q_ref.shape[0]
    q = q_ref[...]
    lane = lax.broadcasted_iota(jnp.int32, q.shape, 1)
    zero = jnp.zeros_like(q)
    both = jnp.concatenate(
        [jnp.where(lane < width // 2, q, zero), jnp.where(lane < width // 2, zero, q)], axis=0
    )
    scores = lax.dot_general(
        both, k_ref[...], (((1,), (1,)), ((), ())), preferred_element_type=F32
    )
    top = jnp.max(scores, axis=1, keepdims=True)
    weights = jnp.exp(scores - top).astype(BF16)
    values = v_ref[...]
    extended = jnp.concatenate([values, jnp.ones_like(values)], axis=1)
    mixed = jnp.dot(weights, extended, preferred_element_type=F32)
    ratio = mixed[:, :width] / mixed[:, width:]
    out = ratio[:rows] - lam_ref[head] * ratio[rows:]
    norm = lax.rsqrt(jnp.mean(out * out, axis=1, keepdims=True) + 1e-05)
    o_ref[...] = (out * norm * gain_ref[...]).astype(BF16)


def rms(x, epsilon):
    return x * lax.rsqrt(jnp.mean(x * x, axis=1, keepdims=True) + epsilon)


def project_kernel(*refs, heads, experts):
    head_refs = refs[:heads]
    w_ref, res_ref, mg_ref, cg_ref, routes_ref, stream_ref = refs[heads : heads + 6]
    out_refs = refs[heads + 6 : heads + 6 + experts]
    acc_ref = refs[-1]
    step = pl.program_id(0)
    width = head_refs[0].shape[2]
    per_step = w_ref.shape[0] // (heads * width)
    lhs = jnp.concatenate(
        [head_refs[j][step * per_step + g] for g in range(per_step) for j in range(heads)], axis=1
    )
    update = jnp.dot(lhs, w_ref[...], preferred_element_type=F32)

    @pl.when(step == 0)
    def _():
        acc_ref[...] = update

    @pl.when(step != 0)
    def _():
        acc_ref[...] += update

    @pl.when(step == pl.num_programs(0) - 1)
    def _():
        stream = (res_ref[...].astype(F32) + rms(acc_ref[...], 1e-06) * mg_ref[...]).astype(BF16)
        stream_ref[...] = stream
        normed = (rms(stream.astype(F32), 1e-06) * cg_ref[...]).astype(BF16)
        tokens = stream.shape[0]
        expert_id = lax.broadcasted_iota(jnp.int32, (experts, tokens), 0)
        named = expert_id == routes_ref[0:1, :]
        for j in range(1, routes_ref.shape[0]):
            named = named | (expert_id == routes_ref[j : j + 1, :])
        before = lax.broadcasted_iota(jnp.int32, (tokens, tokens), 0) < lax.broadcasted_iota(
            jnp.int32, (tokens, tokens), 1
        )
        rank = jnp.dot(
            named.astype(F32).astype(BF16),
            before.astype(F32).astype(BF16),
            preferred_element_type=F32,
        )
        rank = jnp.where(named, rank, -1.0)
        slots = out_refs[0].shape[0]
        slot = lax.broadcasted_iota(jnp.int32, (slots, tokens), 0).astype(F32)
        select = jnp.concatenate(
            [(slot == rank[e : e + 1, :]).astype(F32) for e in range(experts)], axis=0
        ).astype(BF16)
        rows = jnp.dot(select, normed, preferred_element_type=F32).astype(BF16)
        for e in range(experts):
            out_refs[e][...] = rows[e * slots : (e + 1) * slots, :]


def expert_kernel(*refs, pieces):
    x_refs = refs[:pieces]
    g_ref, u_ref, d_ref, mine_ref, theirs_ref = refs[pieces:]
    size = x_refs[0].shape[0]
    rows = jnp.concatenate([x[...] for x in x_refs], axis=0)
    units = g_ref.shape[2]
    block = math.gcd(units, 256)
    parts = []
    for f in range(units // block):
        at = slice(f * block, (f + 1) * block)
        gate = jnp.dot(rows, g_ref[0, :, at], preferred_element_type=F32)
        up = jnp.dot(rows, u_ref[0, :, at], preferred_element_type=F32)
        parts.append((gate / (1.0 + jnp.exp(-gate)) * up).astype(BF16))
    hidden = jnp.concatenate(parts, axis=1)
    half = pieces // 2
    model_dim = d_ref.shape[2]
    block = math.gcd(model_dim, 512)
    for n in range(model_dim // block):
        at = slice(n * block, (n + 1) * block)
        out = jnp.dot(hidden, d_ref[0, :, at], preferred_element_type=F32).astype(BF16)
        for i in range(half):
            mine_ref[i, :, at] = out[i * size : (i + 1) * size, :]
            theirs_ref[i, :, at] = out[(half + i) * size : (half + i + 1) * size, :]


def combine_kernel(*refs, experts):
    back_refs = refs[:experts]
    stream_ref, routes_ref, logits_ref, gain_ref, out_ref = refs[experts:]
    tokens = stream_ref.shape[0]
    top = routes_ref.shape[1]
    slots = back_refs[0].shape[0]
    rows = jnp.concatenate([r[...] for r in back_refs], axis=0)
    expert_id = lax.broadcasted_iota(jnp.int32, (tokens, experts), 1)
    hits = [expert_id == routes_ref[:, j : j + 1] for j in range(top)]
    named = functools.reduce(jnp.logical_or, hits)
    after = lax.broadcasted_iota(jnp.int32, (tokens, tokens), 1) < lax.broadcasted_iota(
        jnp.int32, (tokens, tokens), 0
    )
    rank = jnp.dot(
        after.astype(F32).astype(BF16), named.astype(F32).astype(BF16), preferred_element_type=F32
    )
    logits = logits_ref[...]
    powers = jnp.exp(logits - jnp.max(logits, axis=1, keepdims=True))
    shares = powers / jnp.sum(powers, axis=1, keepdims=True)
    column = lax.broadcasted_iota(jnp.int32, (tokens, experts * slots), 1)
    combined = None
    for j in range(top):
        slot = jnp.sum(jnp.where(hits[j], rank, 0.0), axis=1, keepdims=True).astype(jnp.int32)
        place = routes_ref[:, j : j + 1] * slots + slot
        select = (column == place).astype(F32).astype(BF16)
        picked = jnp.dot(select, rows, preferred_element_type=F32) * shares[:, j : j + 1]
        combined = picked if combined is None else combined + picked
    out_ref[...] = (stream_ref[...].astype(F32) + rms(combined, 1e-06) * gain_ref[...]).astype(BF16)


def local(
    queries,
    key_rows,
    value_rows,
    lambdas,
    head_gain,
    out_weight,
    residual,
    mixer_gain,
    channel_gain,
    expert_gain,
    routes,
    route_logits,
    gate_weight,
    up_weight,
    down_weight,
):
    sp_count = lax.axis_size("sp")
    dp_count = lax.axis_size("dp")
    heads = lambdas.shape[0]
    width = head_gain.shape[0]
    head_dim = width // 2
    tokens, model_dim = residual.shape[1:]
    all_width = queries.shape[2]
    length = tokens * sp_count
    scale = head_dim**-0.5

    lane = jnp.arange(width)
    inverse = 1.0 / 10000.0 ** (
        (2 * (lane % (head_dim // 2))).astype(F32) / head_dim
    )
    position = lax.axis_index("sp") * tokens + jnp.arange(tokens)
    angles = position.astype(F32)[:, None] * inverse[None, :]
    cosine = jnp.cos(angles)
    signed_sine = jnp.where((lane % head_dim < head_dim // 2)[None, :], -1.0, 1.0) * jnp.sin(angles)

    lay_steps = 4
    lay_groups = sp_count // lay_steps
    columns = pl.BlockSpec((None, tokens, all_width // lay_steps), lambda i: (0, 0, i))
    table = pl.BlockSpec((tokens, width), lambda i: (0, 0))
    outgoing = pl.pallas_call(
        functools.partial(layout_kernel, scale=scale),
        grid=(lay_steps,),
        in_specs=[table, table, columns, columns, columns],
        out_specs=[
            pl.BlockSpec((lay_groups, tokens, 3 * width), lambda i: (i, 0, 0))
            for _ in range(heads)
        ],
        out_shape=[
            jax.ShapeDtypeStruct((sp_count, tokens, 3 * width), BF16) for _ in range(heads)
        ],
        compiler_params=params(),
        name="lay",
    )(cosine, signed_sine, queries, key_rows, value_rows)

    gain_row = head_gain.reshape(1, width)
    block = math.gcd(length, 256)
    token_heads = []
    for j in range(heads):
        arrived = lax.all_to_all(outgoing[j], "sp", split_axis=0, concat_axis=0, tiled=True)
        arrived = arrived.reshape(length, 3 * width)
        head_out = pl.pallas_call(
            functools.partial(attention_kernel, head=j),
            grid=(length // block,),
            in_specs=[
                pl.BlockSpec(memory_space=pltpu.SMEM),
                pl.BlockSpec((1, width), lambda i: (0, 0)),
                pl.BlockSpec((block, width), lambda i: (i, 0)),
                pl.BlockSpec((length, width), lambda i: (0, 1)),
                pl.BlockSpec((length, width), lambda i: (0, 2)),
            ],
            out_specs=pl.BlockSpec((block, width), lambda i: (i, 0)),
            out_shape=jax.ShapeDtypeStruct((length, width), BF16),
            compiler_params=params(),
            cost_estimate=pl.CostEstimate(
                flops=8 * length * length * width,
                bytes_accessed=8 * length * width,
                transcendentals=2 * length * length,
            ),
            name=f"attend{j}",
        )(lambdas, gain_row, arrived, arrived, arrived)
        token_heads.append(
            lax.all_to_all(
                head_out.reshape(sp_count, tokens, width),
                "sp",
                split_axis=0,
                concat_axis=0,
                tiled=True,
            )
        )

    experts = sp_count
    capacity = max(2, 3 * tokens // experts)
    top = routes.shape[2]
    own = lax.axis_index("sp")
    paired = sp_count & (sp_count - 1) == 0
    if paired:
        relative = routes.reshape(tokens, top) ^ own
    else:
        relative = (routes.reshape(tokens, top) - own) % sp_count

    def away(k):
        return [(i, i ^ k if paired else (i + k) % sp_count) for i in range(sp_count)]

    def back(k):
        return [(d, s) for s, d in away(k)]

    steps = 4
    k_rows = all_width // steps
    row_spec = pl.BlockSpec((1, model_dim), lambda i: (0, 0))
    full = pl.BlockSpec((tokens, model_dim), lambda i: (0, 0))
    results = pl.pallas_call(
        functools.partial(project_kernel, heads=heads, experts=experts),
        grid=(steps,),
        in_specs=[pl.BlockSpec((sp_count, tokens, width), lambda i: (0, 0, 0))] * heads
        + [
            pl.BlockSpec((k_rows, model_dim), lambda i: (i, 0)),
            full,
            row_spec,
            row_spec,
            pl.BlockSpec((top, tokens), lambda i: (0, 0)),
        ],
        out_specs=[full] + [pl.BlockSpec((capacity, model_dim), lambda i: (0, 0))] * experts,
        out_shape=[jax.ShapeDtypeStruct((tokens, model_dim), BF16)]
        + [jax.ShapeDtypeStruct((capacity, model_dim), BF16)] * experts,
        scratch_shapes=[pltpu.VMEM((tokens, model_dim), F32)],
        compiler_params=params(),
        cost_estimate=pl.CostEstimate(
            flops=2 * tokens * all_width * model_dim,
            bytes_accessed=2 * all_width * model_dim,
            transcendentals=0,
        ),
        name="project",
    )(
        *token_heads,
        out_weight,
        residual.reshape(tokens, model_dim),
        mixer_gain.reshape(1, model_dim),
        channel_gain.reshape(1, model_dim),
        relative.T,
    )
    stream, sent = results[0], results[1:]

    rows_y = dp_count // 2
    core_swap = [(i, i ^ 1) for i in range(dp_count)]

    def shift(k):
        return [(i, ((i // 2 + k) % rows_y) * 2 + i % 2) for i in range(dp_count)]

    pieces = 2 * rows_y
    hidden = gate_weight.shape[2]
    gate_near, up_near, down_near = on_chip(gate_weight), on_chip(up_weight), on_chip(down_weight)
    vmem = pl.BlockSpec(memory_space=pltpu.VMEM)

    def spread(blocks):
        rows = jnp.concatenate(blocks, axis=0)
        here = [rows] + [lax.ppermute(rows, "dp", shift(k)) for k in range(1, rows_y)]
        return here + [lax.ppermute(r, "dp", core_swap) for r in here]

    def expert(rows):
        size = rows[0].shape[0]
        return pl.pallas_call(
            functools.partial(expert_kernel, pieces=pieces),
            in_specs=[vmem] * (pieces + 3),
            out_specs=[vmem] * 2,
            out_shape=[jax.ShapeDtypeStruct((rows_y, size, model_dim), BF16)] * 2,
            compiler_params=params(),
            cost_estimate=pl.CostEstimate(
                flops=6 * pieces * size * model_dim * hidden,
                bytes_accessed=4 * pieces * size * model_dim,
                transcendentals=pieces * size * hidden,
            ),
            name="expert",
        )(*[on_chip(r) for r in rows], gate_near, up_near, down_near)

    def gather_sums(mine, theirs):
        other = lax.ppermute(theirs, "dp", core_swap)
        total = mine[0].astype(F32) + other[0].astype(F32)
        for k in range(1, rows_y):
            pair = (mine[k].astype(F32) + other[k].astype(F32)).astype(BF16)
            total = total + lax.ppermute(pair, "dp", shift(rows_y - k)).astype(F32)
        return total.astype(BF16)

    groups = [(k, k + 1) for k in range(0, sp_count, 2)]
    order = groups[:1] + groups[len(groups) // 2 :] + groups[1 : len(groups) // 2]
    arrived = {}
    for group in order:
        for k in group:
            arrived[k] = lax.ppermute(sent[k], "sp", away(k)) if k else sent[k]
    returned = {}
    for group in order:
        total = gather_sums(*expert(spread([arrived[k] for k in group])))
        for n, k in enumerate(group):
            block = total[n * capacity : (n + 1) * capacity]
            returned[k] = lax.ppermute(block, "sp", back(k)) if k else block

    updated = pl.pallas_call(
        functools.partial(combine_kernel, experts=experts),
        out_shape=jax.ShapeDtypeStruct((tokens, model_dim), BF16),
        compiler_params=params(),
        name="combine",
    )(
        *[returned[k] for k in range(experts)],
        stream,
        relative,
        route_logits.reshape(tokens, top),
        expert_gain.reshape(1, model_dim),
    )
    return updated.reshape(1, tokens, model_dim)


def solution(mesh):
    placed = (
        P("dp", "sp", None),
        P("dp", "sp", None),
        P("dp", "sp", None),
        P("sp"),
        P(),
        P(),
        P("dp", "sp", None),
        P(),
        P(),
        P(),
        P("dp", "sp", None),
        P("dp", "sp", None),
        P("sp", None, "dp"),
        P("sp", None, "dp"),
        P("sp", "dp", None),
    )
    return jax.shard_map(
        local, mesh=mesh, in_specs=placed, out_specs=P("dp", "sp", None), check_vma=False
    )
```

```python
import functools
import math

import jax
import jax.numpy as jnp
from jax import lax
from jax.experimental import pallas as pl
from jax.experimental.pallas import tpu as pltpu
from jax.sharding import PartitionSpec as P


PRICE = 32

F32 = jnp.float32
BF16 = jnp.bfloat16


def params(megabytes=24, **kwargs):
    return pltpu.CompilerParams(vmem_limit_bytes=megabytes * 1024 * 1024, **kwargs)


def on_chip(x):
    return pltpu.with_memory_space_constraint(x, pltpu.VMEM)


def layout_kernel(
    own_ref, cos_ref, sin_ref, q_ref, k_ref, v_ref, first_ref, *near_refs, scale, paired
):
    width = cos_ref.shape[1]
    count = first_ref.shape[0]
    heads = q_ref.shape[2] // (width * count)
    quarter = width // 4
    cosine = cos_ref[...]
    signed_sine = sin_ref[...]
    lane = lax.broadcasted_iota(jnp.int32, cosine.shape, 1)
    front = (lane % (width // 2)) < quarter
    own = own_ref[0]

    def turn(x, factor):
        x = x.astype(F32)
        partner = jnp.where(front, pltpu.roll(x, width - quarter, 1), pltpu.roll(x, quarter, 1))
        return (x * cosine + partner * signed_sine).astype(BF16) * jnp.asarray(factor, BF16)

    for j in range(heads - 1, -1, -1):
        for k in range(count):
            place = (own ^ k if paired else (own + k) % count) if j else k
            at = pl.ds(pl.multiple_of((place * heads + j) * width, width), width)
            parts = turn(q_ref[0, :, at], scale), turn(k_ref[0, :, at], 1.0), v_ref[0, :, at]
            for n, part in enumerate(parts):
                lanes = slice(n * width, (n + 1) * width)
                if j:
                    near_refs[(j - 1) * count + k][:, lanes] = part
                else:
                    first_ref[k, :, lanes] = part


def attention_kernel(own_ref, lam_ref, gain_ref, *refs, head, paired):
    in_refs, o_ref = refs[:-1], refs[-1]
    relative = len(in_refs) > 1
    count = o_ref.shape[0]
    width = o_ref.shape[2]

    def part(k, n):
        at = slice(n * width, (n + 1) * width)
        return in_refs[k][:, at] if relative else in_refs[0][k, :, at]

    keys = jnp.concatenate([part(k, 1) for k in range(count)], axis=0)
    values = jnp.concatenate([part(k, 2) for k in range(count)], axis=0)
    extended = jnp.concatenate([values, jnp.ones_like(values)], axis=1)
    gain = gain_ref[...]
    weight = lam_ref[head]
    own = own_ref[0]
    for pair in range(count // 2):
        q = jnp.concatenate([part(2 * pair, 0), part(2 * pair + 1, 0)], axis=0)
        rows = q.shape[0]
        lane = lax.broadcasted_iota(jnp.int32, q.shape, 1)
        zero = jnp.zeros_like(q)
        both = jnp.concatenate(
            [jnp.where(lane < width // 2, q, zero), jnp.where(lane < width // 2, zero, q)], axis=0
        )
        scores = lax.dot_general(
            both, keys, (((1,), (1,)), ((), ())), preferred_element_type=F32
        )
        top = jnp.max(scores, axis=1, keepdims=True)
        weights = jnp.exp(scores - top).astype(BF16)
        mixed = jnp.dot(weights, extended, preferred_element_type=F32)
        ratio = mixed[:, :width] / mixed[:, width:]
        out = ratio[:rows] - weight * ratio[rows:]
        norm = lax.rsqrt(jnp.mean(out * out, axis=1, keepdims=True) + 1e-05)
        out = (out * norm * gain).astype(BF16)
        for n in range(2):
            k = 2 * pair + n
            if relative:
                k = own ^ k if paired else (own - k + count) % count
            o_ref[k] = out[n * (rows // 2) : (n + 1) * (rows // 2), :]


def rms(x, epsilon):
    return x * lax.rsqrt(jnp.mean(x * x, axis=1, keepdims=True) + epsilon)


def partial_kernel(*refs):
    head_ref, w_ref, out_ref = refs[0], refs[1], refs[-1]
    step = pl.program_id(0)
    count = w_ref.shape[0]
    lhs = jnp.concatenate([head_ref[step * count + g] for g in range(count)], axis=1)
    rhs = jnp.concatenate([w_ref[g] for g in range(count)], axis=0)
    update = jnp.dot(lhs, rhs, preferred_element_type=F32)

    @pl.when(step == 0)
    def _():
        out_ref[...] = update + refs[2][...] if len(refs) > 3 else update

    @pl.when(step != 0)
    def _():
        out_ref[...] += update


def project_kernel(*refs, carried, experts):
    head_ref, w_ref, res_ref, mg_ref, cg_ref, routes_ref = refs[:6]
    stream_ref = refs[6 + carried]
    out_refs = refs[7 + carried : 7 + carried + experts]
    acc_ref = refs[-1]
    step = pl.program_id(0)
    partial_kernel(head_ref, w_ref, *refs[6 : 6 + carried], acc_ref)

    @pl.when(step == pl.num_programs(0) - 1)
    def _():
        stream = (res_ref[...].astype(F32) + rms(acc_ref[...], 1e-06) * mg_ref[...]).astype(BF16)
        stream_ref[...] = stream
        normed = (rms(stream.astype(F32), 1e-06) * cg_ref[...]).astype(BF16)
        tokens = stream.shape[0]
        expert_id = lax.broadcasted_iota(jnp.int32, (experts, tokens), 0)
        named = expert_id == routes_ref[0:1, :]
        for j in range(1, routes_ref.shape[0]):
            named = named | (expert_id == routes_ref[j : j + 1, :])
        before = lax.broadcasted_iota(jnp.int32, (tokens, tokens), 0) < lax.broadcasted_iota(
            jnp.int32, (tokens, tokens), 1
        )
        rank = jnp.dot(
            named.astype(F32).astype(BF16),
            before.astype(F32).astype(BF16),
            preferred_element_type=F32,
        )
        rank = jnp.where(named, rank, -1.0)
        slots = out_refs[0].shape[0]
        slot = lax.broadcasted_iota(jnp.int32, (slots, tokens), 0).astype(F32)
        select = jnp.concatenate(
            [(slot == rank[e : e + 1, :]).astype(F32) for e in range(experts)], axis=0
        ).astype(BF16)
        rows = jnp.dot(select, normed, preferred_element_type=F32).astype(BF16)
        for e in range(experts):
            out_refs[e][...] = rows[e * slots : (e + 1) * slots, :]


def expert_kernel(*refs, pieces):
    x_refs = refs[:pieces]
    g_ref, u_ref, d_ref, mine_ref, theirs_ref = refs[pieces:]
    size = x_refs[0].shape[0]
    rows = jnp.concatenate([x[...] for x in x_refs], axis=0)
    units = g_ref.shape[2]
    block = math.gcd(units, 256)
    parts = []
    for f in range(units // block):
        at = slice(f * block, (f + 1) * block)
        gate = jnp.dot(rows, g_ref[0, :, at], preferred_element_type=F32)
        up = jnp.dot(rows, u_ref[0, :, at], preferred_element_type=F32)
        parts.append((gate / (1.0 + jnp.exp(-gate)) * up).astype(BF16))
    hidden = jnp.concatenate(parts, axis=1)
    half = pieces // 2
    model_dim = d_ref.shape[2]
    block = math.gcd(model_dim, 512)
    for n in range(model_dim // block):
        at = slice(n * block, (n + 1) * block)
        out = jnp.dot(hidden, d_ref[0, :, at], preferred_element_type=F32).astype(BF16)
        for i in range(half):
            mine_ref[i, :, at] = out[i * size : (i + 1) * size, :]
            theirs_ref[i, :, at] = out[(half + i) * size : (half + i + 1) * size, :]


def combine_kernel(*refs, experts):
    back_refs = refs[:experts]
    stream_ref, routes_ref, logits_ref, gain_ref, out_ref = refs[experts:]
    tokens = stream_ref.shape[0]
    top = routes_ref.shape[1]
    slots = back_refs[0].shape[0]
    rows = jnp.concatenate([r[...] for r in back_refs], axis=0)
    expert_id = lax.broadcasted_iota(jnp.int32, (tokens, experts), 1)
    hits = [expert_id == routes_ref[:, j : j + 1] for j in range(top)]
    named = functools.reduce(jnp.logical_or, hits)
    after = lax.broadcasted_iota(jnp.int32, (tokens, tokens), 1) < lax.broadcasted_iota(
        jnp.int32, (tokens, tokens), 0
    )
    rank = jnp.dot(
        after.astype(F32).astype(BF16), named.astype(F32).astype(BF16), preferred_element_type=F32
    )
    logits = logits_ref[...]
    powers = jnp.exp(logits - jnp.max(logits, axis=1, keepdims=True))
    shares = powers / jnp.sum(powers, axis=1, keepdims=True)
    column = lax.broadcasted_iota(jnp.int32, (tokens, experts * slots), 1)
    combined = None
    for j in range(top):
        slot = jnp.sum(jnp.where(hits[j], rank, 0.0), axis=1, keepdims=True).astype(jnp.int32)
        place = routes_ref[:, j : j + 1] * slots + slot
        select = (column == place).astype(F32).astype(BF16)
        picked = jnp.dot(select, rows, preferred_element_type=F32) * shares[:, j : j + 1]
        combined = picked if combined is None else combined + picked
    out_ref[...] = (stream_ref[...].astype(F32) + rms(combined, 1e-06) * gain_ref[...]).astype(BF16)


def group_list(sp_count):
    pairs = [(k, k + 1) for k in range(0, sp_count, 2)]
    return pairs[:1] + pairs[len(pairs) // 2 :][::-1] + pairs[1 : len(pairs) // 2]


def local(
    queries,
    key_rows,
    value_rows,
    lambdas,
    head_gain,
    out_weight,
    residual,
    mixer_gain,
    channel_gain,
    expert_gain,
    routes,
    route_logits,
    gate_weight,
    up_weight,
    down_weight,
):
    sp_count = lax.axis_size("sp")
    dp_count = lax.axis_size("dp")
    heads = lambdas.shape[0]
    width = head_gain.shape[0]
    head_dim = width // 2
    tokens, model_dim = residual.shape[1:]
    length = tokens * sp_count
    scale = head_dim**-0.5

    lane = jnp.arange(width)
    inverse = 1.0 / 10000.0 ** (
        (2 * (lane % (head_dim // 2))).astype(F32) / head_dim
    )
    position = lax.axis_index("sp") * tokens + jnp.arange(tokens)
    angles = position.astype(F32)[:, None] * inverse[None, :]
    cosine = jnp.cos(angles)
    signed_sine = jnp.where((lane % head_dim < head_dim // 2)[None, :], -1.0, 1.0) * jnp.sin(angles)

    own = lax.axis_index("sp")
    own_row = own.reshape(1)
    paired = sp_count & (sp_count - 1) == 0

    def away(k):
        return [(i, i ^ k if paired else (i + k) % sp_count) for i in range(sp_count)]

    def back(k):
        return [(d, s) for s, d in away(k)]

    vmem = pl.BlockSpec(memory_space=pltpu.VMEM)
    smem = pl.BlockSpec(memory_space=pltpu.SMEM)
    near = (heads - 1) * sp_count
    outgoing = pl.pallas_call(
        functools.partial(layout_kernel, scale=scale, paired=paired),
        grid=(1,),
        in_specs=[smem, pl.BlockSpec((tokens, width), lambda i: (0, 0))]
        + [pl.BlockSpec((tokens, width), lambda i: (0, 0))]
        + [pl.BlockSpec(queries.shape, lambda i: (0, 0, 0))] * 3,
        out_specs=[vmem] * (1 + near),
        out_shape=[jax.ShapeDtypeStruct((sp_count, tokens, 3 * width), BF16)]
        + [jax.ShapeDtypeStruct((tokens, 3 * width), BF16)] * near,
        compiler_params=params(12),
        name="lay",
    )(
        own_row,
        cosine,
        signed_sine,
        *[pltpu.with_memory_space_constraint(x, pltpu.HBM) for x in (queries, key_rows, value_rows)],
    )

    gain_row = head_gain.reshape(1, width)
    arrived = [
        [lax.all_to_all(outgoing[0], "sp", split_axis=0, concat_axis=0, tiled=True)]
    ]
    for j in range(1, heads):
        blocks = list(outgoing[1 + (j - 1) * sp_count : 1 + j * sp_count])
        for k in range(1, sp_count):
            blocks[k] = lax.ppermute(blocks[k], "sp", away(k))
        arrived.append(blocks)
    weight_view = pltpu.with_memory_space_constraint(
        out_weight.reshape(sp_count, heads, width, model_dim), pltpu.HBM
    )
    steps = 4
    count = sp_count // steps
    full = pl.BlockSpec((tokens, model_dim), lambda i: (0, 0))
    head_spec = pl.BlockSpec((sp_count, tokens, width), lambda i: (0, 0, 0))
    carry = []
    for j in [*range(1, heads), 0]:
        head_out = pl.pallas_call(
            functools.partial(attention_kernel, head=j, paired=paired),
            in_specs=[smem, smem] + [vmem] * (1 + len(arrived[j])),
            out_specs=vmem,
            out_shape=jax.ShapeDtypeStruct((sp_count, tokens, width), BF16),
            compiler_params=params(16),
            cost_estimate=pl.CostEstimate(
                flops=8 * length * length * width,
                bytes_accessed=8 * length * width,
                transcendentals=2 * length * length,
            ),
        )(own_row, lambdas, gain_row, *[on_chip(x) for x in arrived[j]])
        token_head = lax.all_to_all(
            head_out, "sp", split_axis=0, concat_axis=0, tiled=True
        )
        weight_spec = pl.BlockSpec(
            (count, None, width, model_dim), functools.partial(lambda i, j: (i, j, 0, 0), j=j)
        )
        if j:
            carry = [
                pl.pallas_call(
                    partial_kernel,
                    grid=(steps,),
                    in_specs=[head_spec, weight_spec] + [full] * len(carry),
                    out_specs=full,
                    out_shape=jax.ShapeDtypeStruct((tokens, model_dim), F32),
                    compiler_params=params(12),
                    cost_estimate=pl.CostEstimate(
                        flops=2 * tokens * sp_count * width * model_dim,
                        bytes_accessed=2 * sp_count * width * model_dim,
                        transcendentals=0,
                    ),
                )(token_head, weight_view, *carry)
            ]

    experts = sp_count
    capacity = max(2, 3 * tokens // experts)
    top = routes.shape[2]
    if paired:
        relative = routes.reshape(tokens, top) ^ own
    else:
        relative = (routes.reshape(tokens, top) - own) % sp_count

    row_spec = pl.BlockSpec((1, model_dim), lambda i: (0, 0))
    results = pl.pallas_call(
        functools.partial(project_kernel, carried=len(carry), experts=experts),
        grid=(steps,),
        in_specs=[
            head_spec,
            weight_spec,
            full,
            row_spec,
            row_spec,
            pl.BlockSpec((top, tokens), lambda i: (0, 0)),
        ]
        + [full] * len(carry),
        out_specs=[full] + [pl.BlockSpec((capacity, model_dim), lambda i: (0, 0))] * experts,
        out_shape=[jax.ShapeDtypeStruct((tokens, model_dim), BF16)]
        + [jax.ShapeDtypeStruct((capacity, model_dim), BF16)] * experts,
        scratch_shapes=[pltpu.VMEM((tokens, model_dim), F32)],
        compiler_params=params(14),
        cost_estimate=pl.CostEstimate(
            flops=PRICE * tokens * sp_count * width * model_dim,
            bytes_accessed=PRICE * sp_count * width * model_dim,
            transcendentals=0,
        ),
        name="project",
    )(
        token_head,
        weight_view,
        residual.reshape(tokens, model_dim),
        mixer_gain.reshape(1, model_dim),
        channel_gain.reshape(1, model_dim),
        relative.T,
        *carry,
    )
    stream, sent = results[0], results[1:]

    rows_y = dp_count // 2
    core_swap = [(i, i ^ 1) for i in range(dp_count)]

    def shift(k):
        return [(i, ((i // 2 + k) % rows_y) * 2 + i % 2) for i in range(dp_count)]

    pieces = 2 * rows_y
    hidden = gate_weight.shape[2]
    gate_near, up_near, down_near = on_chip(gate_weight), on_chip(up_weight), on_chip(down_weight)

    def spread(blocks):
        rows = jnp.concatenate(blocks, axis=0)
        here = [rows]
        for k in range(1, rows_y):
            here.append(lax.ppermute(rows, "dp", shift(k)))
        there = []
        for r in here:
            there.append(lax.ppermute(r, "dp", core_swap))
        return here + there

    def expert(rows):
        size = rows[0].shape[0]
        return pl.pallas_call(
            functools.partial(expert_kernel, pieces=pieces),
            in_specs=[vmem] * (pieces + 3),
            out_specs=[vmem] * 2,
            out_shape=[jax.ShapeDtypeStruct((rows_y, size, model_dim), BF16)] * 2,
            compiler_params=params(),
            cost_estimate=pl.CostEstimate(
                flops=6 * pieces * size * model_dim * hidden,
                bytes_accessed=4 * pieces * size * model_dim,
                transcendentals=pieces * size * hidden,
            ),
        )(*[on_chip(r) for r in rows], gate_near, up_near, down_near)

    def gather_sums(mine, theirs):
        other = lax.ppermute(theirs, "dp", core_swap)
        total = mine[0].astype(F32) + other[0].astype(F32)
        for k in range(1, rows_y):
            pair = (mine[k].astype(F32) + other[k].astype(F32)).astype(BF16)
            got = lax.ppermute(pair, "dp", shift(rows_y - k))
            total = total + got.astype(F32)
        return total.astype(BF16)

    groups = group_list(sp_count)
    arrived = {}
    for group in groups:
        for k in group:
            arrived[k] = lax.ppermute(sent[k], "sp", away(k)) if k else sent[k]
    returned = {}
    for group in groups:
        parts = expert(spread([arrived[k] for k in group]))
        total = gather_sums(*parts)
        for n, k in enumerate(group):
            block = total[n * capacity : (n + 1) * capacity]
            returned[k] = lax.ppermute(block, "sp", back(k)) if k else block

    updated = pl.pallas_call(
        functools.partial(combine_kernel, experts=experts),
        out_shape=jax.ShapeDtypeStruct((tokens, model_dim), BF16),
        compiler_params=params(12),
        name="combine",
    )(
        *[returned[k] for k in range(experts)],
        stream,
        relative,
        route_logits.reshape(tokens, top),
        expert_gain.reshape(1, model_dim),
    )
    return updated.reshape(1, tokens, model_dim)


def solution(mesh):
    placed = (
        P("dp", "sp", None),
        P("dp", "sp", None),
        P("dp", "sp", None),
        P("sp"),
        P(),
        P(),
        P("dp", "sp", None),
        P(),
        P(),
        P(),
        P("dp", "sp", None),
        P("dp", "sp", None),
        P("sp", None, "dp"),
        P("sp", None, "dp"),
        P("sp", "dp", None),
    )

    return jax.shard_map(
        local, mesh=mesh, in_specs=placed, out_specs=P("dp", "sp", None), check_vma=False
    )
```

```python
import functools
import math

import jax
import jax.numpy as jnp
from jax import lax
from jax.experimental import pallas as pl
from jax.experimental.pallas import tpu as pltpu
from jax.sharding import PartitionSpec as P


PRICE = 64

F32 = jnp.float32
BF16 = jnp.bfloat16


def params(megabytes=24, **kwargs):
    return pltpu.CompilerParams(vmem_limit_bytes=megabytes * 1024 * 1024, **kwargs)


def on_chip(x):
    return pltpu.with_memory_space_constraint(x, pltpu.VMEM)


def layout_kernel(
    own_ref, cos_ref, sin_ref, q_ref, k_ref, v_ref, first_ref, *near_refs, scale, paired
):
    width = cos_ref.shape[1]
    count = first_ref.shape[0]
    heads = q_ref.shape[2] // (width * count)
    quarter = width // 4
    cosine = cos_ref[...]
    signed_sine = sin_ref[...]
    lane = lax.broadcasted_iota(jnp.int32, cosine.shape, 1)
    front = (lane % (width // 2)) < quarter
    own = own_ref[0]

    def turn(x, factor):
        x = x.astype(F32)
        partner = jnp.where(front, pltpu.roll(x, width - quarter, 1), pltpu.roll(x, quarter, 1))
        return (x * cosine + partner * signed_sine).astype(BF16) * jnp.asarray(factor, BF16)

    for j in range(heads - 1, -1, -1):
        for k in range(count):
            place = (own ^ k if paired else (own + k) % count) if j else k
            at = pl.ds(pl.multiple_of((place * heads + j) * width, width), width)
            parts = turn(q_ref[0, :, at], scale), turn(k_ref[0, :, at], 1.0), v_ref[0, :, at]
            for n, part in enumerate(parts):
                lanes = slice(n * width, (n + 1) * width)
                if j:
                    near_refs[(j - 1) * count + k][:, lanes] = part
                else:
                    first_ref[k, :, lanes] = part


def attention_kernel(lam_ref, gain_ref, *refs, head):
    relative = len(refs) > 2
    half = len(refs) // 2
    in_refs, o_refs = refs[:half], refs[half:]
    count = len(o_refs) if relative else o_refs[0].shape[0]
    width = o_refs[0].shape[-1]

    def part(k, n):
        at = slice(n * width, (n + 1) * width)
        return in_refs[k][:, at] if relative else in_refs[0][k, :, at]

    keys = jnp.concatenate([part(k, 1) for k in range(count)], axis=0)
    values = jnp.concatenate([part(k, 2) for k in range(count)], axis=0)
    extended = jnp.concatenate([values, jnp.ones_like(values)], axis=1)
    gain = gain_ref[...]
    weight = lam_ref[head]
    for pair in range(count // 2):
        q = jnp.concatenate([part(2 * pair, 0), part(2 * pair + 1, 0)], axis=0)
        rows = q.shape[0]
        lane = lax.broadcasted_iota(jnp.int32, q.shape, 1)
        zero = jnp.zeros_like(q)
        both = jnp.concatenate(
            [jnp.where(lane < width // 2, q, zero), jnp.where(lane < width // 2, zero, q)], axis=0
        )
        scores = lax.dot_general(
            both, keys, (((1,), (1,)), ((), ())), preferred_element_type=F32
        )
        top = jnp.max(scores, axis=1, keepdims=True)
        weights = jnp.exp(scores - top).astype(BF16)
        mixed = jnp.dot(weights, extended, preferred_element_type=F32)
        ratio = mixed[:, :width] / mixed[:, width:]
        out = ratio[:rows] - weight * ratio[rows:]
        norm = lax.rsqrt(jnp.mean(out * out, axis=1, keepdims=True) + 1e-05)
        out = (out * norm * gain).astype(BF16)
        for n in range(2):
            k = 2 * pair + n
            if relative:
                o_refs[k][...] = out[n * (rows // 2) : (n + 1) * (rows // 2), :]
            else:
                o_refs[0][k] = out[n * (rows // 2) : (n + 1) * (rows // 2), :]


def rms(x, epsilon):
    return x * lax.rsqrt(jnp.mean(x * x, axis=1, keepdims=True) + epsilon)


def partial_kernel(*refs):
    head_ref, w_ref, out_ref = refs[0], refs[1], refs[-1]
    step = pl.program_id(0)
    count = w_ref.shape[0]
    lhs = jnp.concatenate([head_ref[step * count + g] for g in range(count)], axis=1)
    rhs = jnp.concatenate([w_ref[g] for g in range(count)], axis=0)
    update = jnp.dot(lhs, rhs, preferred_element_type=F32)

    @pl.when(step == 0)
    def _():
        out_ref[...] = update + refs[2][...] if len(refs) > 3 else update

    @pl.when(step != 0)
    def _():
        out_ref[...] += update


def near_kernel(own_ref, *refs, per_step):
    del own_ref
    head_refs, w_refs, out_ref = refs[: -per_step - 1], refs[-per_step - 1 : -1], refs[-1]
    step = pl.program_id(0)
    rhs = jnp.concatenate([w[0, 0] for w in w_refs], axis=0)
    for i in range(len(head_refs) // per_step):

        @pl.when(step == i)
        def _(i=i):
            lhs = jnp.concatenate([r[...] for r in head_refs[i * per_step : (i + 1) * per_step]], axis=1)
            update = jnp.dot(lhs, rhs, preferred_element_type=F32)
            if i:
                out_ref[...] += update
            else:
                out_ref[...] = update


def project_kernel(*refs, carried, experts):
    head_ref, w_ref, res_ref, mg_ref, cg_ref, routes_ref = refs[:6]
    stream_ref = refs[6 + carried]
    out_refs = refs[7 + carried : 7 + carried + experts]
    acc_ref = refs[-1]
    step = pl.program_id(0)
    partial_kernel(head_ref, w_ref, *refs[6 : 6 + carried], acc_ref)

    @pl.when(step == pl.num_programs(0) - 1)
    def _():
        stream = (res_ref[...].astype(F32) + rms(acc_ref[...], 1e-06) * mg_ref[...]).astype(BF16)
        stream_ref[...] = stream
        normed = (rms(stream.astype(F32), 1e-06) * cg_ref[...]).astype(BF16)
        tokens = stream.shape[0]
        expert_id = lax.broadcasted_iota(jnp.int32, (experts, tokens), 0)
        named = expert_id == routes_ref[0:1, :]
        for j in range(1, routes_ref.shape[0]):
            named = named | (expert_id == routes_ref[j : j + 1, :])
        before = lax.broadcasted_iota(jnp.int32, (tokens, tokens), 0) < lax.broadcasted_iota(
            jnp.int32, (tokens, tokens), 1
        )
        rank = jnp.dot(
            named.astype(F32).astype(BF16),
            before.astype(F32).astype(BF16),
            preferred_element_type=F32,
        )
        rank = jnp.where(named, rank, -1.0)
        slots = out_refs[0].shape[0]
        slot = lax.broadcasted_iota(jnp.int32, (slots, tokens), 0).astype(F32)
        select = jnp.concatenate(
            [(slot == rank[e : e + 1, :]).astype(F32) for e in range(experts)], axis=0
        ).astype(BF16)
        rows = jnp.dot(select, normed, preferred_element_type=F32).astype(BF16)
        for e in range(experts):
            out_refs[e][...] = rows[e * slots : (e + 1) * slots, :]


def expert_kernel(*refs, pieces):
    x_refs = refs[:pieces]
    g_ref, u_ref, d_ref, mine_ref, theirs_ref = refs[pieces:]
    size = x_refs[0].shape[0]
    rows = jnp.concatenate([x[...] for x in x_refs], axis=0)
    units = g_ref.shape[2]
    block = math.gcd(units, 256)
    parts = []
    for f in range(units // block):
        at = slice(f * block, (f + 1) * block)
        gate = jnp.dot(rows, g_ref[0, :, at], preferred_element_type=F32)
        up = jnp.dot(rows, u_ref[0, :, at], preferred_element_type=F32)
        parts.append((gate / (1.0 + jnp.exp(-gate)) * up).astype(BF16))
    hidden = jnp.concatenate(parts, axis=1)
    half = pieces // 2
    model_dim = d_ref.shape[2]
    block = math.gcd(model_dim, 512)
    for n in range(model_dim // block):
        at = slice(n * block, (n + 1) * block)
        out = jnp.dot(hidden, d_ref[0, :, at], preferred_element_type=F32).astype(BF16)
        for i in range(half):
            mine_ref[i, :, at] = out[i * size : (i + 1) * size, :]
            theirs_ref[i, :, at] = out[(half + i) * size : (half + i + 1) * size, :]


def combine_kernel(*refs, experts):
    back_refs = refs[:experts]
    stream_ref, routes_ref, logits_ref, gain_ref, out_ref = refs[experts:]
    tokens = stream_ref.shape[0]
    top = routes_ref.shape[1]
    slots = back_refs[0].shape[0]
    rows = jnp.concatenate([r[...] for r in back_refs], axis=0)
    expert_id = lax.broadcasted_iota(jnp.int32, (tokens, experts), 1)
    hits = [expert_id == routes_ref[:, j : j + 1] for j in range(top)]
    named = functools.reduce(jnp.logical_or, hits)
    after = lax.broadcasted_iota(jnp.int32, (tokens, tokens), 1) < lax.broadcasted_iota(
        jnp.int32, (tokens, tokens), 0
    )
    rank = jnp.dot(
        after.astype(F32).astype(BF16), named.astype(F32).astype(BF16), preferred_element_type=F32
    )
    logits = logits_ref[...]
    powers = jnp.exp(logits - jnp.max(logits, axis=1, keepdims=True))
    shares = powers / jnp.sum(powers, axis=1, keepdims=True)
    column = lax.broadcasted_iota(jnp.int32, (tokens, experts * slots), 1)
    combined = None
    for j in range(top):
        slot = jnp.sum(jnp.where(hits[j], rank, 0.0), axis=1, keepdims=True).astype(jnp.int32)
        place = routes_ref[:, j : j + 1] * slots + slot
        select = (column == place).astype(F32).astype(BF16)
        picked = jnp.dot(select, rows, preferred_element_type=F32) * shares[:, j : j + 1]
        combined = picked if combined is None else combined + picked
    out_ref[...] = (stream_ref[...].astype(F32) + rms(combined, 1e-06) * gain_ref[...]).astype(BF16)


def group_list(sp_count):
    pairs = [(k, k + 1) for k in range(0, sp_count, 2)]
    pairs = [pairs[0]] + [p[::-1] for p in pairs[1:]]
    return pairs[:1] + pairs[len(pairs) // 2 :][::-1] + pairs[1 : len(pairs) // 2]


def local(
    queries,
    key_rows,
    value_rows,
    lambdas,
    head_gain,
    out_weight,
    residual,
    mixer_gain,
    channel_gain,
    expert_gain,
    routes,
    route_logits,
    gate_weight,
    up_weight,
    down_weight,
):
    sp_count = lax.axis_size("sp")
    dp_count = lax.axis_size("dp")
    heads = lambdas.shape[0]
    width = head_gain.shape[0]
    head_dim = width // 2
    tokens, model_dim = residual.shape[1:]
    length = tokens * sp_count
    scale = head_dim**-0.5

    lane = jnp.arange(width)
    inverse = 1.0 / 10000.0 ** (
        (2 * (lane % (head_dim // 2))).astype(F32) / head_dim
    )
    position = lax.axis_index("sp") * tokens + jnp.arange(tokens)
    angles = position.astype(F32)[:, None] * inverse[None, :]
    cosine = jnp.cos(angles)
    signed_sine = jnp.where((lane % head_dim < head_dim // 2)[None, :], -1.0, 1.0) * jnp.sin(angles)

    own = lax.axis_index("sp")
    own_row = own.reshape(1)
    paired = sp_count & (sp_count - 1) == 0

    def away(k):
        return [(i, i ^ k if paired else (i + k) % sp_count) for i in range(sp_count)]

    def back(k):
        return [(d, s) for s, d in away(k)]

    vmem = pl.BlockSpec(memory_space=pltpu.VMEM)
    smem = pl.BlockSpec(memory_space=pltpu.SMEM)
    near = (heads - 1) * sp_count
    outgoing = pl.pallas_call(
        functools.partial(layout_kernel, scale=scale, paired=paired),
        grid=(1,),
        in_specs=[smem, pl.BlockSpec((tokens, width), lambda i: (0, 0))]
        + [pl.BlockSpec((tokens, width), lambda i: (0, 0))]
        + [pl.BlockSpec(queries.shape, lambda i: (0, 0, 0))] * 3,
        out_specs=[vmem] * (1 + near),
        out_shape=[jax.ShapeDtypeStruct((sp_count, tokens, 3 * width), BF16)]
        + [jax.ShapeDtypeStruct((tokens, 3 * width), BF16)] * near,
        compiler_params=params(12),
        name="lay",
    )(
        own_row,
        cosine,
        signed_sine,
        *[pltpu.with_memory_space_constraint(x, pltpu.HBM) for x in (queries, key_rows, value_rows)],
    )

    gain_row = head_gain.reshape(1, width)
    arrived = [
        [lax.all_to_all(outgoing[0], "sp", split_axis=0, concat_axis=0, tiled=True)]
    ]
    for j in range(1, heads):
        blocks = list(outgoing[1 + (j - 1) * sp_count : 1 + j * sp_count])
        for k in range(1, sp_count):
            blocks[k] = lax.ppermute(blocks[k], "sp", away(k))
        arrived.append(blocks)
    weight_view = pltpu.with_memory_space_constraint(
        out_weight.reshape(sp_count, heads, width, model_dim), pltpu.HBM
    )
    steps = 4
    count = sp_count // steps
    full = pl.BlockSpec((tokens, model_dim), lambda i: (0, 0))
    head_spec = pl.BlockSpec((sp_count, tokens, width), lambda i: (0, 0, 0))
    carry = []
    for j in [*range(1, heads), 0]:
        near_head = j > 0
        block = jax.ShapeDtypeStruct((tokens, width), BF16)
        head_out = pl.pallas_call(
            functools.partial(attention_kernel, head=j),
            in_specs=[smem] + [vmem] * (1 + len(arrived[j])),
            out_specs=[vmem] * sp_count if near_head else vmem,
            out_shape=[block] * sp_count
            if near_head
            else jax.ShapeDtypeStruct((sp_count, tokens, width), BF16),
            compiler_params=params(16),
            cost_estimate=pl.CostEstimate(
                flops=PRICE * length * length * width,
                bytes_accessed=8 * length * width,
                transcendentals=2 * length * length,
            ),
        )(lambdas, gain_row, *[on_chip(x) for x in arrived[j]])
        if near_head:
            head_out = list(head_out)
            for k in range(1, sp_count):
                head_out[k] = lax.ppermute(head_out[k], "sp", back(k))
            per_step = 2

            def weight_place(i, o, n=0, j=j):
                k = i * per_step + n
                return (o[0] ^ k if paired else (o[0] + k) % sp_count), j, 0, 0

            carry.append(
                pl.pallas_call(
                    functools.partial(near_kernel, per_step=per_step),
                    grid_spec=pltpu.PrefetchScalarGridSpec(
                        num_scalar_prefetch=1,
                        grid=(sp_count // per_step,),
                        in_specs=[vmem] * sp_count
                        + [
                            pl.BlockSpec(
                                (1, 1, width, model_dim), functools.partial(weight_place, n=n)
                            )
                            for n in range(per_step)
                        ],
                        out_specs=pl.BlockSpec((tokens, model_dim), lambda i, o: (0, 0)),
                    ),
                    out_shape=jax.ShapeDtypeStruct((tokens, model_dim), F32),
                    compiler_params=params(12),
                    cost_estimate=pl.CostEstimate(
                        flops=2 * tokens * sp_count * width * model_dim,
                        bytes_accessed=2 * sp_count * width * model_dim,
                        transcendentals=0,
                    ),
                )(own_row, *[on_chip(x) for x in head_out], weight_view, weight_view)
            )
            continue
        token_head = lax.all_to_all(
            head_out, "sp", split_axis=0, concat_axis=0, tiled=True
        )
        weight_spec = pl.BlockSpec(
            (count, None, width, model_dim), functools.partial(lambda i, j: (i, j, 0, 0), j=j)
        )
    if len(carry) > 1:
        carry = [functools.reduce(jnp.add, carry)]

    experts = sp_count
    capacity = max(2, 3 * tokens // experts)
    top = routes.shape[2]
    if paired:
        relative = routes.reshape(tokens, top) ^ own
    else:
        relative = (routes.reshape(tokens, top) - own) % sp_count

    row_spec = pl.BlockSpec((1, model_dim), lambda i: (0, 0))
    results = pl.pallas_call(
        functools.partial(project_kernel, carried=len(carry), experts=experts),
        grid=(steps,),
        in_specs=[
            head_spec,
            weight_spec,
            full,
            row_spec,
            row_spec,
            pl.BlockSpec((top, tokens), lambda i: (0, 0)),
        ]
        + [full] * len(carry),
        out_specs=[full] + [pl.BlockSpec((capacity, model_dim), lambda i: (0, 0))] * experts,
        out_shape=[jax.ShapeDtypeStruct((tokens, model_dim), BF16)]
        + [jax.ShapeDtypeStruct((capacity, model_dim), BF16)] * experts,
        scratch_shapes=[pltpu.VMEM((tokens, model_dim), F32)],
        compiler_params=params(14),
        cost_estimate=pl.CostEstimate(
            flops=PRICE * tokens * sp_count * width * model_dim,
            bytes_accessed=PRICE * sp_count * width * model_dim,
            transcendentals=0,
        ),
        name="project",
    )(
        token_head,
        weight_view,
        residual.reshape(tokens, model_dim),
        mixer_gain.reshape(1, model_dim),
        channel_gain.reshape(1, model_dim),
        relative.T,
        *carry,
    )
    stream, sent = results[0], results[1:]

    rows_y = dp_count // 2
    core_swap = [(i, i ^ 1) for i in range(dp_count)]

    def shift(k):
        return [(i, ((i // 2 + k) % rows_y) * 2 + i % 2) for i in range(dp_count)]

    pieces = 2 * rows_y
    hidden = gate_weight.shape[2]
    gate_near, up_near, down_near = on_chip(gate_weight), on_chip(up_weight), on_chip(down_weight)

    def spread(blocks):
        rows = jnp.concatenate(blocks, axis=0)
        here = [rows]
        for k in range(1, rows_y):
            here.append(lax.ppermute(rows, "dp", shift(k)))
        there = []
        for r in here:
            there.append(lax.ppermute(r, "dp", core_swap))
        return here + there

    def expert(rows):
        size = rows[0].shape[0]
        return pl.pallas_call(
            functools.partial(expert_kernel, pieces=pieces),
            in_specs=[vmem] * (pieces + 3),
            out_specs=[vmem] * 2,
            out_shape=[jax.ShapeDtypeStruct((rows_y, size, model_dim), BF16)] * 2,
            compiler_params=params(),
            cost_estimate=pl.CostEstimate(
                flops=6 * pieces * size * model_dim * hidden,
                bytes_accessed=4 * pieces * size * model_dim,
                transcendentals=pieces * size * hidden,
            ),
        )(*[on_chip(r) for r in rows], gate_near, up_near, down_near)

    def gather_sums(mine, theirs):
        other = lax.ppermute(theirs, "dp", core_swap)
        total = mine[0].astype(F32) + other[0].astype(F32)
        for k in range(1, rows_y):
            pair = (mine[k].astype(F32) + other[k].astype(F32)).astype(BF16)
            got = lax.ppermute(pair, "dp", shift(rows_y - k))
            total = total + got.astype(F32)
        return total.astype(BF16)

    groups = group_list(sp_count)
    arrived = {}
    for group in groups:
        for k in group:
            arrived[k] = lax.ppermute(sent[k], "sp", away(k)) if k else sent[k]
    returned = {}
    for group in groups:
        parts = expert(spread([arrived[k] for k in group]))
        total = gather_sums(*parts)
        for n, k in enumerate(group):
            block = total[n * capacity : (n + 1) * capacity]
            returned[k] = lax.ppermute(block, "sp", back(k)) if k else block

    updated = pl.pallas_call(
        functools.partial(combine_kernel, experts=experts),
        out_shape=jax.ShapeDtypeStruct((tokens, model_dim), BF16),
        compiler_params=params(12),
        name="combine",
    )(
        *[returned[k] for k in range(experts)],
        stream,
        relative,
        route_logits.reshape(tokens, top),
        expert_gain.reshape(1, model_dim),
    )
    return updated.reshape(1, tokens, model_dim)


def solution(mesh):
    placed = (
        P("dp", "sp", None),
        P("dp", "sp", None),
        P("dp", "sp", None),
        P("sp"),
        P(),
        P(),
        P("dp", "sp", None),
        P(),
        P(),
        P(),
        P("dp", "sp", None),
        P("dp", "sp", None),
        P("sp", None, "dp"),
        P("sp", None, "dp"),
        P("sp", "dp", None),
    )

    return jax.shard_map(
        local, mesh=mesh, in_specs=placed, out_specs=P("dp", "sp", None), check_vma=False
    )
```
